32 devices in a mesh: grp: 2 (over x), ep: 16 (over z, y, core).
Axes of the slice: x: 2, y: 2, z: 4, core: 2. Of those that a mesh axis runs over, the one named last changes fastest.
Arguments:
- tokens: bfloat16 [1024, 2048], P(('grp', 'ep')), parts along dimension 0, may hold values from -6 to 6
- routes: int32 [1024, 4], P(('grp', 'ep')), parts along dimension 0, may hold values from 0 to 15, all different within a row; in each aligned block of 32 rows (0 to 31, 32 to 63, ...) at most 16 rows name the same one
- in_gain: float32 [2048], replicated, may hold values from 0.1 to 1.9
- group_router: float32 [2048, 4], replicated, may hold values from -0.03125 to 0.03125
- expert_router: float32 [2048, 16], replicated, may hold values from -0.03125 to 0.03125
- w_gate: bfloat16 [16, 2048, 512], P('ep'), may hold values from -0.125 to 0.125
- w_up: bfloat16 [16, 2048, 512], P('ep'), may hold values from -0.125 to 0.125
- w_down: bfloat16 [16, 512, 2048], P('ep')
- out_gain: float32 [2048], P('ep'), may hold values from 0.1 to 1.9
Outputs:
- mixed_out: bfloat16 [1024, 2048], P('grp', 'ep'), parts along dimension 0
The draws below stay inside these ranges and needn't reach their ends.
There are 2 independent parts, one for each index of `grp`. The reference program is written for one: setup_inputs(seed, part) draws one part's arguments, and reference() takes and returns one part's arrays. A program takes and returns all parts, laid end to end along the dimension named above; an argument that names none is the same for every part. Nothing has to cross between parts.
Inputs may be any that keep to these rules, and one draw needn't show every extreme that they name: `routes`: each row names 4 different experts; in the rows of one device no expert is named more than 16 times, a bound that some block reaches.
All inputs are finite; a program needn't handle non-finite values.
Results may differ from the reference program's by a relative error of at most 0.0085.
Values may be sent and summed in bfloat16 or wider, within the bound.
A program may use at most 64 MiB of HBM per device.

```python
import math
import jax
import jax.numpy as jnp
import numpy as np
from jax import lax

D = 2048
FF = 512
N_GROUPS = 4
TOPK = 4
TOK_DEV = 32
EXPERTS = 16
TOKENS = 512
CAP = 16
N_EP = 16


def draw_w_down(key, part):
    first, second = jax.random.split(jax.random.fold_in(key, 7))
    column = jnp.arange(D, dtype=jnp.float32) / D
    base = jax.random.normal(first, (EXPERTS, FF, D), jnp.float32)
    rising = (1.0 + 2.0 * column) ** 0.5
    rough = jax.random.uniform(second, (D,), jnp.float32, 0.6, 1.4)
    return (base * FF ** (-0.5) * rising * rough).astype(jnp.bfloat16)


def block_scale(stream_key, shape, cuts, smallest, top_value):
    gain, own = 1.0, jax.random.fold_in(stream_key, 6)
    for axis_at, shards_of in cuts:
        steps = jnp.exp(jax.random.uniform(jax.random.fold_in(own, axis_at), (shards_of,), jnp.float32, smallest / len(cuts), top_value / len(cuts)))
        gain = gain * jnp.repeat(steps, shape[axis_at] // shards_of).reshape([-1 if axis == axis_at else 1 for axis in range(len(shape))])
    return gain


def shared_out(key, own, number, rows, count, top, bound, slope):
    order = jax.random.permutation(key, count)
    packed, usual = portions_of(count, rows * top, bound, slope, True), portions_of(count, rows * top, bound, slope, False)
    places = jnp.arange(count)

    def named(lengths, offset_by):
        used = int((lengths > 0).sum())
        fixed = max(1, used // 4)
        shifted = fixed + (places - fixed + offset_by * (used - fixed)) % max(1, count - fixed)
        return jnp.zeros((count,), jnp.int32).at[order[jnp.where(places < fixed, places, shifted)]].set(jnp.asarray(lengths, jnp.int32))

    lengths = jnp.where(number % 4 == 0, named(packed, number // 4), named(usual, number - number // 4 - 1))
    mixed = jax.random.permutation(jax.random.fold_in(own, 3), count)
    source_of, sink = mixed[0:count // 2 * 2:2], mixed[1:count // 2 * 2:2]
    room = jnp.minimum(lengths[source_of] - 1, bound - lengths[sink]) // 2
    room = jnp.where((source_of == order[0]) | (sink == order[0]) | (lengths[sink] == 0), 0, jnp.maximum(room, 0))
    shifted = jax.random.randint(jax.random.fold_in(own, 4), (count // 2,), 0, 1 << 20) % (room + 1)
    lengths = lengths.at[source_of].add(-shifted).at[sink].add(shifted)
    items = jnp.searchsorted(jnp.cumsum(lengths), jnp.arange(rows * top), side="right").astype(jnp.int32)
    table = items.reshape(top, rows).T
    table = table[jax.random.permutation(jax.random.fold_in(own, 1), rows)]
    offset_by = jax.random.randint(jax.random.fold_in(own, 2), (rows, 1), 0, top)
    return jnp.take_along_axis(table, (jnp.arange(top)[None, :] + offset_by) % top, axis=1)


def portions_of(number_of, total, reach, skew, full):
    loads = [(1 << 20) // math.isqrt(grade ** skew) + 1 for grade in range(1, number_of + 1)]
    largest = reach if full else min(reach, max(-(-total // number_of), total * loads[0] // sum(loads)))
    least = 1 if total - largest >= number_of - 1 else 0
    holding, surplus = [largest] + [least] * (number_of - 1), total - largest - least * (number_of - 1)
    while surplus > 0:
        movable = [i for i in range(1, number_of) if holding[i] < largest] or [i for i in range(1, number_of) if holding[i] < reach]
        mass, budget = sum([loads[i] for i in movable]), surplus
        for i in movable:
            addition = min(reach - holding[i], max(1, budget * loads[i] // mass), surplus)
            holding[i] = holding[i] + addition
            surplus = surplus - addition
    return np.array(holding)


def bell_draw(rng, shape, deviation, most, pieces=(), kind=jnp.bfloat16):
    level = block_scale(rng, shape, pieces, -0.22, 0.18) if pieces else 1.0
    array = jax.random.normal(rng, shape, jnp.float32) * deviation * level
    return jnp.minimum(jnp.maximum(array, -most), most).astype(kind)


def setup_inputs(seed: int = 0, part: int = 0) -> dict:
    key_of = jax.random.split(jax.random.key(seed), 10)
    part_splits = jax.random.split(jax.random.fold_in(key_of[9], part), 10)
    tokens = bell_draw(part_splits[0], (TOKENS, D), 1.0, 6.0, ((0, 16),))
    routes_keys = jax.random.split(jax.random.fold_in(part_splits[1], 1), TOKENS // TOK_DEV)
    routes_turns = jax.random.permutation(jax.random.fold_in(part_splits[1], 3), TOKENS // TOK_DEV)
    routes = jax.vmap(lambda own, number: shared_out(jax.random.fold_in(part_splits[1], 2), own, number, TOK_DEV, EXPERTS, TOPK, CAP, 2))(routes_keys, routes_turns).reshape((TOKENS, TOPK))
    in_gain = jnp.clip(1.0 + 0.18 * jax.random.normal(key_of[2], (D,), jnp.float32), 0.1, 1.9)
    group_router = bell_draw(key_of[3], (D, N_GROUPS), (16 * D) ** -0.5, 0.03125, (), jnp.float32)
    expert_router = bell_draw(key_of[4], (D, EXPERTS), (16 * D) ** -0.5, 0.03125, (), jnp.float32)
    w_gate = bell_draw(key_of[5], (EXPERTS, D, FF), D ** -0.5, 0.125, ((0, 16),))
    w_up = bell_draw(key_of[6], (EXPERTS, D, FF), D ** -0.5, 0.125, ((0, 16),))
    w_down = draw_w_down(jax.random.fold_in(key_of[9], 71), part)
    out_gain = jnp.clip(1.0 + 0.18 * jax.random.normal(key_of[8], (D,), jnp.float32), 0.1, 1.9)
    return {"tokens": tokens, "routes": routes, "in_gain": in_gain, "group_router": group_router, "expert_router": expert_router, "w_gate": w_gate, "w_up": w_up, "w_down": w_down, "out_gain": out_gain}


EPSILON = 1e-06

def expert_rows(rows, gate_mat, up_mat, down_mat):
    gate = jnp.dot(rows, gate_mat, preferred_element_type=jnp.float32)
    upward = jnp.dot(rows, up_mat, preferred_element_type=jnp.float32)
    hidden = (jax.nn.silu(gate) * upward).astype(jnp.bfloat16)
    return jnp.dot(hidden, down_mat, preferred_element_type=jnp.float32).astype(jnp.bfloat16)

def reference(tokens, routes, in_gain, group_router, expert_router, w_gate, w_up, w_down, out_gain):
    values = tokens.astype(jnp.float32)
    normed = (values * lax.rsqrt(lax.optimization_barrier(jnp.mean(values * values, axis=1, keepdims=True)) + EPSILON) * in_gain).astype(jnp.bfloat16)
    wide = normed.astype(jnp.float32)
    group_logit = jnp.dot(wide, group_router, precision=lax.Precision.HIGHEST)
    expert_logit = jnp.dot(wide, expert_router, precision=lax.Precision.HIGHEST)
    group_prob = jnp.exp(group_logit) / lax.optimization_barrier(jnp.sum(jnp.exp(group_logit), axis=1, keepdims=True))
    chosen = jnp.exp(jnp.take_along_axis(expert_logit, routes, axis=1))
    expert_prob = chosen / lax.optimization_barrier(jnp.sum(chosen, axis=1, keepdims=True))
    per_group = EXPERTS // N_GROUPS
    weight = jnp.take_along_axis(group_prob, routes // per_group, axis=1) * expert_prob
    pairs = routes.reshape(N_EP, TOK_DEV * TOPK)
    onehot = (pairs[:, :, None] == jnp.arange(EXPERTS, dtype=jnp.int32)).astype(jnp.int32)
    order_in = lax.optimization_barrier(jnp.sum(onehot * (jnp.cumsum(onehot, axis=1) - 1), axis=2)).astype(jnp.int32)
    slot_index = (jnp.arange(N_EP, dtype=jnp.int32)[:, None] * CAP + order_in).reshape(-1)
    expert_of = routes.reshape(-1)
    token_index = jnp.arange(TOKENS * TOPK, dtype=jnp.int32) // TOPK
    table = jnp.zeros((EXPERTS, N_EP * CAP), jnp.int32).at[expert_of, slot_index].set(token_index)
    answers = lax.map(lambda group: expert_rows(normed[group[0]], group[1], group[2], group[3]), (table, w_gate, w_up, w_down))
    pair_rows = answers[expert_of, slot_index].astype(jnp.float32)
    mixed = lax.optimization_barrier(jnp.sum((pair_rows * weight.reshape(-1)[:, None]).reshape(TOKENS, TOPK, D), axis=1))
    scale = lax.rsqrt(lax.optimization_barrier(jnp.mean(mixed * mixed, axis=1, keepdims=True)) + EPSILON)
    return (mixed * scale * out_gain).astype(jnp.bfloat16)
```

```python
import functools

import jax
import jax.numpy as jnp
from jax import lax
from jax.experimental import pallas as pl
from jax.experimental.pallas import tpu as pltpu
from jax.sharding import PartitionSpec as P

EPSILON = 1e-06
LANES = 128
CORES = 2
HIGH = lax.Precision.HIGHEST
UP, DOWN, SIDE, CORE = 0, 1, 2, 3


def target_of(step, z, depth):
    mirrored = z * 2 > depth - 1
    near = jnp.where(mirrored, depth - 1 - z, z)
    lone = depth - 1 - 2 * near
    paired = step - lone
    apart = near - paired // 2
    far = jnp.where(paired % 2 == 0, near + apart, near - apart)
    found = jnp.where(step < lone, depth - 1 - step, far)
    return jnp.where(mirrored, depth - 1 - found, found)


def kernel(
    n, tokens, routes, in_gain, group_router, expert_router, w_gate, w_up, w_down, out_gain,
    out, gate_w, up_w, down_w, rows, turned, hidden, held, core_out, core_in, side_out, side_in,
    line_out, up_in, down_in, squares, total,
    load_sem, row_sent, row_got, core_sent, core_got, side_sent, side_got,
    line_sent, up_got, down_got, square_sent, square_got,
):
    tok_dev, width = tokens.shape
    experts = expert_router.shape[0]
    groups = group_router.shape[0]
    sides = 2 if (n // CORES) % 2 == 0 else 1
    plane = sides * CORES
    depth = n // plane
    ntok = n * tok_dev
    block = width // n
    ff = gate_w.shape[1]
    me = lax.axis_index("ep")
    z, y, c = me // plane, (me // CORES) % sides, me % CORES
    side_step, core_step = (1 - 2 * y) * CORES, 1 - 2 * c

    loads = [
        pltpu.make_async_copy(src.at[0], dst, load_sem.at[i])
        for i, (src, dst) in enumerate(((w_gate, gate_w), (w_up, up_w), (w_down, down_w)))
    ]
    for load in loads:
        load.start()

    barrier = pltpu.get_barrier_semaphore()

    def greet(k, carry):
        pl.semaphore_signal(
            barrier, inc=1, device_id={"ep": (me + k) % n}, device_id_type=pl.DeviceIdType.MESH
        )
        return carry

    lax.fori_loop(1, n, greet, 0)

    values = tokens[...].astype(jnp.float32)
    scaled = values * lax.rsqrt(jnp.mean(values * values, axis=1, keepdims=True) + EPSILON)
    normed = (scaled * in_gain[...]).astype(jnp.bfloat16)
    rows[me, :, :width] = normed
    wide = normed.astype(jnp.float32)
    across = (((1,), (1,)), ((), ()))
    group_logit = lax.dot_general(
        group_router[...], wide, across, precision=HIGH, preferred_element_type=jnp.float32
    )
    expert_logit = lax.dot_general(
        expert_router[...], wide, across, precision=HIGH, preferred_element_type=jnp.float32
    )
    group_exp = jnp.exp(group_logit)
    group_prob = group_exp / jnp.sum(group_exp, axis=0, keepdims=True)
    number = lax.broadcasted_iota(jnp.int32, (experts, tok_dev), 0)
    named = number == routes[0:1, :]
    for j in range(1, routes.shape[0]):
        named = named | (number == routes[j : j + 1, :])
    chosen = jnp.where(named, jnp.exp(expert_logit), 0.0)
    weight = chosen / jnp.sum(chosen, axis=0, keepdims=True)
    per_group = experts // groups
    of_group = jnp.zeros_like(weight)
    for g in range(groups):
        inside = (number >= g * per_group) & (number < (g + 1) * per_group)
        of_group = jnp.where(inside, group_prob[g : g + 1, :], of_group)
    weight = weight * of_group
    high = weight.astype(jnp.bfloat16).astype(jnp.float32)
    turned[...] = jnp.zeros_like(turned)
    turned[:experts, :tok_dev] = high
    turned[experts : 2 * experts, :tok_dev] = weight - high
    rows[me, :, width:] = turned[...].T[:tok_dev, :].astype(jnp.bfloat16)

    pl.semaphore_wait(barrier, n - 1)

    def row_copy(slot, way, device):
        return pltpu.make_async_remote_copy(
            src_ref=rows.at[slot], dst_ref=rows.at[slot],
            send_sem=row_sent.at[way, slot], recv_sem=row_got.at[slot],
            device_id={"ep": device}, device_id_type=pl.DeviceIdType.MESH,
        )

    def to_side(slot):
        if sides > 1:
            row_copy(slot, SIDE, me + side_step).start()

    def to_core(slot):
        row_copy(slot, CORE, me + core_step).start()

    def to_up(slot):
        @pl.when(z < depth - 1)
        def _():
            row_copy(slot, UP, me + plane).start()

    def to_down(slot):
        @pl.when(z > 0)
        def _():
            row_copy(slot, DOWN, me - plane).start()

    def got(slot):
        row_copy(slot, CORE, me + core_step).wait_recv()

    to_up(me)
    to_down(me)
    to_side(me)
    to_core(me)

    def from_side(k):
        if sides > 1:
            @pl.when(z - k >= 0)
            def _():
                slot = me - k * plane + side_step
                got(slot)
                to_core(slot)

            if k > 0:
                @pl.when(z + k < depth)
                def _():
                    slot = me + k * plane + side_step
                    got(slot)
                    to_core(slot)

    for k in range(1, depth):
        @pl.when(z - k >= 0)
        def _():
            slot = me - k * plane
            got(slot)
            to_up(slot)
            to_side(slot)
            to_core(slot)

        @pl.when(z + k < depth)
        def _():
            slot = me + k * plane
            got(slot)
            to_down(slot)
            to_side(slot)
            to_core(slot)

        from_side(k - 1)
    from_side(depth - 1)

    def from_core(k, carry):
        got(k * CORES + 1 - c)
        return carry

    lax.fori_loop(0, n // CORES, from_core, 0)

    loads[0].wait()
    loads[1].wait()
    lane = lax.broadcasted_iota(jnp.int32, (ntok, LANES), 1)
    mine = (lane == me) | (lane == experts + me)
    spread = rows[:, :, width:].reshape(ntok, LANES).astype(jnp.float32)
    column = jnp.sum(jnp.where(mine, spread, 0.0), axis=1, keepdims=True)
    tile = min(256, ff)

    def forward(i, carry):
        at = pl.ds(pl.multiple_of(i * tile, tile), tile)
        arrived = rows[:, :, :width].reshape(ntok, width)
        gate = jnp.dot(arrived, gate_w[:, at], preferred_element_type=jnp.float32)
        upward = jnp.dot(arrived, up_w[:, at], preferred_element_type=jnp.float32)
        silu = gate / (1.0 + jnp.exp(-gate))
        hidden[:, at] = (silu * upward * column).astype(jnp.bfloat16)
        return carry

    lax.fori_loop(0, ff // tile, forward, 0)
    loads[2].wait()

    def core_copy(j):
        return pltpu.make_async_remote_copy(
            src_ref=core_out.at[j], dst_ref=core_in.at[j],
            send_sem=core_sent.at[j], recv_sem=core_got.at[j],
            device_id={"ep": me + core_step}, device_id_type=pl.DeviceIdType.MESH,
        )

    def side_copy(j):
        return pltpu.make_async_remote_copy(
            src_ref=side_out.at[j], dst_ref=side_in.at[j],
            send_sem=side_sent.at[j], recv_sem=side_got.at[j],
            device_id={"ep": me + side_step}, device_id_type=pl.DeviceIdType.MESH,
        )

    def up_copy(target):
        return pltpu.make_async_remote_copy(
            src_ref=line_out.at[target], dst_ref=up_in.at[target],
            send_sem=line_sent.at[target], recv_sem=up_got.at[target],
            device_id={"ep": me + plane}, device_id_type=pl.DeviceIdType.MESH,
        )

    def down_copy(target):
        return pltpu.make_async_remote_copy(
            src_ref=line_out.at[target], dst_ref=down_in.at[target],
            send_sem=line_sent.at[target], recv_sem=down_got.at[target],
            device_id={"ep": me - plane}, device_id_type=pl.DeviceIdType.MESH,
        )

    def produce(j):
        span = plane * block
        at = pl.ds(pl.multiple_of(target_of(j, z, depth) * span, span), span)
        answer = jnp.dot(hidden[...], down_w[:, at], preferred_element_type=jnp.float32)
        for s in range(sides):
            first = answer[:, s * CORES * block : (s * CORES + 1) * block]
            second = answer[:, (s * CORES + 1) * block : (s + 1) * CORES * block]
            held[j, s] = jnp.where(c == 0, first, second)
            core_out[j, s] = jnp.where(c == 0, second, first).astype(jnp.bfloat16)
        core_copy(j).start()

    def pair(j):
        core_copy(j).wait_recv()
        held[j, y] = held[j, y] + core_in[j, y].astype(jnp.float32)
        if sides > 1:
            far = held[j, 1 - y] + core_in[j, 1 - y].astype(jnp.float32)
            side_out[j] = far.astype(jnp.bfloat16)
            side_copy(j).start()

    produce(0)

    def produce_pair(j, carry):
        produce(j)
        pair(j - 1)
        return carry

    lax.fori_loop(1, depth, produce_pair, 0)
    pair(depth - 1)

    def plane_sum(j):
        found = held[j, y]
        if sides > 1:
            side_copy(j).wait_recv()
            found = found + side_in[j].astype(jnp.float32)
        return found

    def line(j, carry):
        target = target_of(j, z, depth)
        held[j, y] = plane_sum(j)

        @pl.when(target > z)
        def _():
            @pl.when(z > 0)
            def _():
                up_copy(target).wait_recv()
                held[j, y] = held[j, y] + up_in[target].astype(jnp.float32)

            line_out[target] = held[j, y].astype(jnp.bfloat16)
            up_copy(target).start()

        @pl.when(target < z)
        def _():
            @pl.when(z < depth - 1)
            def _():
                down_copy(target).wait_recv()
                held[j, y] = held[j, y] + down_in[target].astype(jnp.float32)

            line_out[target] = held[j, y].astype(jnp.bfloat16)
            down_copy(target).start()

        return carry

    lax.fori_loop(0, depth - 1, line, 0)
    total[...] = plane_sum(depth - 1)

    @pl.when(z > 0)
    def _():
        up_copy(z).wait_recv()
        total[...] = total[...] + up_in[z].astype(jnp.float32)

    @pl.when(z < depth - 1)
    def _():
        down_copy(z).wait_recv()
        total[...] = total[...] + down_in[z].astype(jnp.float32)

    mixed = total[...]
    summed = lax.dot_general(
        jnp.ones((8, block), jnp.float32), mixed * mixed, across,
        precision=HIGH, preferred_element_type=jnp.float32,
    )
    squares[me] = summed[0:1, :]

    def square_copy(slot, device):
        return pltpu.make_async_remote_copy(
            src_ref=squares.at[slot], dst_ref=squares.at[slot],
            send_sem=square_sent.at[device], recv_sem=square_got.at[slot],
            device_id={"ep": device}, device_id_type=pl.DeviceIdType.MESH,
        )

    def square_start(k, carry):
        square_copy(me, (me + k) % n).start()
        return carry

    lax.fori_loop(1, n, square_start, 0)

    def row_done(k, carry):
        slot = k * plane + y * CORES + c
        row_copy(slot, CORE, me + core_step).wait_send()
        if sides > 1:
            row_copy(slot, SIDE, me + side_step).wait_send()
            row_copy(slot + side_step, CORE, me + core_step).wait_send()

        @pl.when((k <= z) & (z < depth - 1))
        def _():
            row_copy(slot, UP, me + plane).wait_send()

        @pl.when((k >= z) & (z > 0))
        def _():
            row_copy(slot, DOWN, me - plane).wait_send()

        core_copy(k).wait_send()
        if sides > 1:
            side_copy(k).wait_send()

        @pl.when(k > z)
        def _():
            up_copy(k).wait_send()

        @pl.when(k < z)
        def _():
            down_copy(k).wait_send()

        return carry

    lax.fori_loop(0, depth, row_done, 0)

    def square_wait(k, carry):
        square_copy((me + k) % n, (me + k) % n).wait_recv()
        return carry

    lax.fori_loop(1, n, square_wait, 0)
    power = jnp.sum(squares[...], axis=0)
    tall = jnp.broadcast_to(power, (LANES, ntok)).T[:, :block]
    scale = lax.rsqrt(tall / width + EPSILON)
    out[...] = (total[...] * scale * out_gain[...]).astype(jnp.bfloat16)

    def square_done(k, carry):
        square_copy(me, (me + k) % n).wait_send()
        return carry

    lax.fori_loop(1, n, square_done, 0)


def per_device(
    n, tokens, routes, in_gain, group_router, expert_router, w_gate, w_up, w_down, out_gain
):
    tok_dev, width = tokens.shape
    ff = w_gate.shape[2]
    ntok, block = n * tok_dev, width // n
    sides = 2 if (n // CORES) % 2 == 0 else 1
    depth = n // (sides * CORES)
    bf16, f32 = jnp.bfloat16, jnp.float32
    dma = pltpu.SemaphoreType.DMA
    vmem = pl.BlockSpec(memory_space=pltpu.VMEM)
    hbm = pl.BlockSpec(memory_space=pl.ANY)
    return pl.pallas_call(
        functools.partial(kernel, n),
        out_shape=jax.ShapeDtypeStruct((ntok, block), bf16),
        in_specs=[vmem] * 5 + [hbm] * 3 + [vmem],
        out_specs=vmem,
        scratch_shapes=[
            pltpu.VMEM((width, ff), bf16),
            pltpu.VMEM((width, ff), bf16),
            pltpu.VMEM((ff, width), bf16),
            pltpu.VMEM((n, tok_dev, width + LANES), bf16),
            pltpu.VMEM((LANES, LANES), f32),
            pltpu.VMEM((ntok, ff), bf16),
            pltpu.VMEM((depth, sides, ntok, block), f32),
            pltpu.VMEM((depth, sides, ntok, block), bf16),
            pltpu.VMEM((depth, sides, ntok, block), bf16),
            pltpu.VMEM((depth, ntok, block), bf16),
            pltpu.VMEM((depth, ntok, block), bf16),
            pltpu.VMEM((depth, ntok, block), bf16),
            pltpu.VMEM((depth, ntok, block), bf16),
            pltpu.VMEM((depth, ntok, block), bf16),
            pltpu.VMEM((n, 1, ntok), f32),
            pltpu.VMEM((ntok, block), f32),
            dma((3,)),
            dma((4, n)),
            dma((n,)),
            dma((depth,)),
            dma((depth,)),
            dma((depth,)),
            dma((depth,)),
            dma((depth,)),
            dma((depth,)),
            dma((depth,)),
            dma((n,)),
            dma((n,)),
        ],
        compiler_params=pltpu.CompilerParams(
            collective_id=0, has_side_effects=True, vmem_limit_bytes=60 * 1024 * 1024
        ),
    )(
        tokens, routes.T, in_gain.reshape(1, width), group_router.T, expert_router.T,
        w_gate, w_up, w_down, out_gain.reshape(1, block),
    )


def solution(mesh):
    in_specs = (
        P(("grp", "ep"), None),
        P(("grp", "ep"), None),
        P(),
        P(),
        P(),
        P("ep", None, None),
        P("ep", None, None),
        P("ep", None, None),
        P("ep"),
    )
    return jax.shard_map(
        functools.partial(per_device, mesh.shape["ep"]),
        mesh=mesh, in_specs=in_specs, out_specs=P("grp", "ep"), check_vma=False,
    )
```

```python
import functools

import jax
import jax.numpy as jnp
from jax import lax
from jax.experimental import pallas as pl
from jax.experimental.pallas import tpu as pltpu
from jax.sharding import PartitionSpec as P

EPSILON = 1e-06
LANES = 128
CORES = 2
HIGH = lax.Precision.HIGHEST
UP, DOWN, SIDE, CORE = 0, 1, 2, 3
ROW_PIECES = 2
SUM_PIECES = 2


def target_of(step, z, depth):
    mirrored = z * 2 > depth - 1
    near = jnp.where(mirrored, depth - 1 - z, z)
    lone = depth - 1 - 2 * near
    paired = step - lone
    apart = near - paired // 2
    far = jnp.where(paired % 2 == 0, near + apart, near - apart)
    found = jnp.where(step < lone, depth - 1 - step, far)
    return jnp.where(mirrored, depth - 1 - found, found)


def kernel(
    n, tokens, routes, in_gain, group_router, expert_router, w_gate, w_up, w_down, out_gain,
    out, gate_w, up_w, down_w, rows, turned, hidden, held, core_out, core_in, side_out, side_in,
    line_out, up_in, down_in, squares, total,
    load_sem, row_sent, row_got, core_sent, core_got, side_sent, side_got,
    line_sent, up_got, down_got, square_sent, square_got,
):
    tok_dev, width = tokens.shape
    experts = expert_router.shape[0]
    groups = group_router.shape[0]
    sides = 2 if (n // CORES) % 2 == 0 else 1
    plane = sides * CORES
    depth = n // plane
    ntok = n * tok_dev
    block = width // n
    ff = gate_w.shape[1]
    piece = tok_dev // ROW_PIECES
    part = ntok // SUM_PIECES
    me = lax.axis_index("ep")
    z, y, c = me // plane, (me // CORES) % sides, me % CORES
    side_step, core_step = (1 - 2 * y) * CORES, 1 - 2 * c

    loads = [
        pltpu.make_async_copy(src.at[0], dst, load_sem.at[i])
        for i, (src, dst) in enumerate(((w_gate, gate_w), (w_up, up_w), (w_down, down_w)))
    ]
    for load in loads:
        load.start()

    barrier = pltpu.get_barrier_semaphore()

    def greet(k, carry):
        pl.semaphore_signal(
            barrier, inc=1, device_id={"ep": (me + k) % n}, device_id_type=pl.DeviceIdType.MESH
        )
        return carry

    lax.fori_loop(1, n, greet, 0)

    values = tokens[...].astype(jnp.float32)
    scaled = values * lax.rsqrt(jnp.mean(values * values, axis=1, keepdims=True) + EPSILON)
    normed = (scaled * in_gain[...]).astype(jnp.bfloat16)
    rows[me, :, :width] = normed
    wide = normed.astype(jnp.float32)
    across = (((1,), (1,)), ((), ()))
    group_logit = lax.dot_general(
        group_router[...], wide, across, precision=HIGH, preferred_element_type=jnp.float32
    )
    expert_logit = lax.dot_general(
        expert_router[...], wide, across, precision=HIGH, preferred_element_type=jnp.float32
    )
    group_exp = jnp.exp(group_logit)
    group_prob = group_exp / jnp.sum(group_exp, axis=0, keepdims=True)
    number = lax.broadcasted_iota(jnp.int32, (experts, tok_dev), 0)
    named = number == routes[0:1, :]
    for j in range(1, routes.shape[0]):
        named = named | (number == routes[j : j + 1, :])
    chosen = jnp.where(named, jnp.exp(expert_logit), 0.0)
    weight = chosen / jnp.sum(chosen, axis=0, keepdims=True)
    per_group = experts // groups
    of_group = jnp.zeros_like(weight)
    for g in range(groups):
        inside = (number >= g * per_group) & (number < (g + 1) * per_group)
        of_group = jnp.where(inside, group_prob[g : g + 1, :], of_group)
    weight = weight * of_group
    high = weight.astype(jnp.bfloat16).astype(jnp.float32)
    turned[...] = jnp.zeros_like(turned)
    turned[:experts, :tok_dev] = high
    turned[experts : 2 * experts, :tok_dev] = weight - high
    rows[me, :, width:] = turned[...].T[:tok_dev, :].astype(jnp.bfloat16)

    pl.semaphore_wait(barrier, n - 1)

    def row_copy(slot, p, way, device):
        at = rows.at[slot, pl.ds(p * piece, piece)]
        return pltpu.make_async_remote_copy(
            src_ref=at, dst_ref=at,
            send_sem=row_sent.at[way, slot, p], recv_sem=row_got.at[slot, p],
            device_id={"ep": device}, device_id_type=pl.DeviceIdType.MESH,
        )

    def to_side(slot, p):
        if sides > 1:
            row_copy(slot, p, SIDE, me + side_step).start()

    def to_core(slot, p):
        row_copy(slot, p, CORE, me + core_step).start()

    def to_up(slot, p):
        @pl.when(z < depth - 1)
        def _():
            row_copy(slot, p, UP, me + plane).start()

    def to_down(slot, p):
        @pl.when(z > 0)
        def _():
            row_copy(slot, p, DOWN, me - plane).start()

    def got(slot, p):
        row_copy(slot, p, CORE, me + core_step).wait_recv()

    for p in range(ROW_PIECES):
        to_up(me, p)
        to_down(me, p)
        to_side(me, p)
    for p in range(ROW_PIECES):
        to_core(me, p)

    def from_side(k, p):
        if sides > 1:
            @pl.when(z - k >= 0)
            def _():
                slot = me - k * plane + side_step
                got(slot, p)
                to_core(slot, p)

            if k > 0:
                @pl.when(z + k < depth)
                def _():
                    slot = me + k * plane + side_step
                    got(slot, p)
                    to_core(slot, p)

    for k in range(1, depth):
        for p in range(ROW_PIECES):
            @pl.when(z - k >= 0)
            def _():
                slot = me - k * plane
                got(slot, p)
                to_up(slot, p)
                to_side(slot, p)
                to_core(slot, p)

            @pl.when(z + k < depth)
            def _():
                slot = me + k * plane
                got(slot, p)
                to_down(slot, p)
                to_side(slot, p)
                to_core(slot, p)

            if k > 1:
                from_side(k - 2, p)
    for k in range(max(depth - 2, 0), depth):
        for p in range(ROW_PIECES):
            from_side(k, p)

    def from_core(k, carry):
        for p in range(ROW_PIECES):
            got(k * CORES + 1 - c, p)
        return carry

    lax.fori_loop(0, n // CORES, from_core, 0)

    loads[0].wait()
    loads[1].wait()
    lane = lax.broadcasted_iota(jnp.int32, (ntok, LANES), 1)
    mine = (lane == me) | (lane == experts + me)
    spread = rows[:, :, width:].reshape(ntok, LANES).astype(jnp.float32)
    column = jnp.sum(jnp.where(mine, spread, 0.0), axis=1, keepdims=True)
    tile = min(256, ff)

    def forward(i, carry):
        at = pl.ds(pl.multiple_of(i * tile, tile), tile)
        arrived = rows[:, :, :width].reshape(ntok, width)
        gate = jnp.dot(arrived, gate_w[:, at], preferred_element_type=jnp.float32)
        upward = jnp.dot(arrived, up_w[:, at], preferred_element_type=jnp.float32)
        silu = gate / (1.0 + jnp.exp(-gate))
        hidden[:, at] = (silu * upward * column).astype(jnp.bfloat16)
        return carry

    lax.fori_loop(0, ff // tile, forward, 0)
    loads[2].wait()

    def core_copy(j):
        return pltpu.make_async_remote_copy(
            src_ref=core_out.at[j], dst_ref=core_in.at[j],
            send_sem=core_sent.at[j], recv_sem=core_got.at[j],
            device_id={"ep": me + core_step}, device_id_type=pl.DeviceIdType.MESH,
        )

    def side_copy(j):
        return pltpu.make_async_remote_copy(
            src_ref=side_out.at[j], dst_ref=side_in.at[j],
            send_sem=side_sent.at[j], recv_sem=side_got.at[j],
            device_id={"ep": me + side_step}, device_id_type=pl.DeviceIdType.MESH,
        )

    def up_copy(target):
        return pltpu.make_async_remote_copy(
            src_ref=line_out.at[target], dst_ref=up_in.at[target],
            send_sem=line_sent.at[target], recv_sem=up_got.at[target],
            device_id={"ep": me + plane}, device_id_type=pl.DeviceIdType.MESH,
        )

    def down_copy(target):
        return pltpu.make_async_remote_copy(
            src_ref=line_out.at[target], dst_ref=down_in.at[target],
            send_sem=line_sent.at[target], recv_sem=down_got.at[target],
            device_id={"ep": me - plane}, device_id_type=pl.DeviceIdType.MESH,
        )

    units = depth * SUM_PIECES

    def produce(u):
        span = plane * block
        target = target_of(u // SUM_PIECES, z, depth)
        at = pl.ds(pl.multiple_of(target * span, span), span)
        some = pl.ds(pl.multiple_of(u % SUM_PIECES * part, part), part)
        answer = jnp.dot(hidden[some, :], down_w[:, at], preferred_element_type=jnp.float32)
        for s in range(sides):
            first = answer[:, s * CORES * block : (s * CORES + 1) * block]
            second = answer[:, (s * CORES + 1) * block : (s + 1) * CORES * block]
            held[u, s] = jnp.where(c == 0, first, second)
            core_out[u, s] = jnp.where(c == 0, second, first).astype(jnp.bfloat16)
        core_copy(u).start()

    def pair(u):
        core_copy(u).wait_recv()
        held[u, y] = held[u, y] + core_in[u, y].astype(jnp.float32)
        if sides > 1:
            far = held[u, 1 - y] + core_in[u, 1 - y].astype(jnp.float32)
            side_out[u] = far.astype(jnp.bfloat16)
            side_copy(u).start()

    produce(0)

    def produce_pair(u, carry):
        produce(u)
        pair(u - 1)
        return carry

    lax.fori_loop(1, units, produce_pair, 0)
    pair(units - 1)

    def plane_sum(u):
        found = held[u, y]
        if sides > 1:
            side_copy(u).wait_recv()
            found = found + side_in[u].astype(jnp.float32)
        return found

    def line(u, carry):
        target = target_of(u // SUM_PIECES, z, depth)
        spot = target * SUM_PIECES + u % SUM_PIECES
        held[u, y] = plane_sum(u)

        @pl.when(target > z)
        def _():
            @pl.when(z > 0)
            def _():
                up_copy(spot).wait_recv()
                held[u, y] = held[u, y] + up_in[spot].astype(jnp.float32)

            line_out[spot] = held[u, y].astype(jnp.bfloat16)
            up_copy(spot).start()

        @pl.when(target < z)
        def _():
            @pl.when(z < depth - 1)
            def _():
                down_copy(spot).wait_recv()
                held[u, y] = held[u, y] + down_in[spot].astype(jnp.float32)

            line_out[spot] = held[u, y].astype(jnp.bfloat16)
            down_copy(spot).start()

        return carry

    lax.fori_loop(0, units - SUM_PIECES, line, 0)
    for p in range(SUM_PIECES):
        spot = z * SUM_PIECES + p
        some = pl.ds(p * part, part)
        total[some, :] = plane_sum(units - SUM_PIECES + p)

        @pl.when(z > 0)
        def _():
            up_copy(spot).wait_recv()
            total[some, :] = total[some, :] + up_in[spot].astype(jnp.float32)

        @pl.when(z < depth - 1)
        def _():
            down_copy(spot).wait_recv()
            total[some, :] = total[some, :] + down_in[spot].astype(jnp.float32)

    mixed = total[...]
    summed = lax.dot_general(
        jnp.ones((8, block), jnp.float32), mixed * mixed, across,
        precision=HIGH, preferred_element_type=jnp.float32,
    )
    squares[me] = summed[0:1, :]

    def square_copy(slot, device):
        return pltpu.make_async_remote_copy(
            src_ref=squares.at[slot], dst_ref=squares.at[slot],
            send_sem=square_sent.at[device], recv_sem=square_got.at[slot],
            device_id={"ep": device}, device_id_type=pl.DeviceIdType.MESH,
        )

    def square_start(k, carry):
        square_copy(me, (me + k) % n).start()
        return carry

    lax.fori_loop(1, n, square_start, 0)

    def row_done(k, carry):
        slot = k * plane + y * CORES + c
        for p in range(ROW_PIECES):
            row_copy(slot, p, CORE, me + core_step).wait_send()
            if sides > 1:
                row_copy(slot, p, SIDE, me + side_step).wait_send()
                row_copy(slot + side_step, p, CORE, me + core_step).wait_send()

            @pl.when((k <= z) & (z < depth - 1))
            def _():
                row_copy(slot, p, UP, me + plane).wait_send()

            @pl.when((k >= z) & (z > 0))
            def _():
                row_copy(slot, p, DOWN, me - plane).wait_send()

        return carry

    lax.fori_loop(0, depth, row_done, 0)

    def sum_done(u, carry):
        k = u // SUM_PIECES
        core_copy(u).wait_send()
        if sides > 1:
            side_copy(u).wait_send()

        @pl.when(k > z)
        def _():
            up_copy(u).wait_send()

        @pl.when(k < z)
        def _():
            down_copy(u).wait_send()

        return carry

    lax.fori_loop(0, depth * SUM_PIECES, sum_done, 0)

    def square_wait(k, carry):
        square_copy((me + k) % n, (me + k) % n).wait_recv()
        return carry

    lax.fori_loop(1, n, square_wait, 0)
    power = jnp.sum(squares[...], axis=0)
    tall = jnp.broadcast_to(power, (LANES, ntok)).T[:, :block]
    scale = lax.rsqrt(tall / width + EPSILON)
    out[...] = (total[...] * scale * out_gain[...]).astype(jnp.bfloat16)

    def square_done(k, carry):
        square_copy(me, (me + k) % n).wait_send()
        return carry

    lax.fori_loop(1, n, square_done, 0)


def per_device(
    n, tokens, routes, in_gain, group_router, expert_router, w_gate, w_up, w_down, out_gain
):
    tok_dev, width = tokens.shape
    ff = w_gate.shape[2]
    ntok, block = n * tok_dev, width // n
    sides = 2 if (n // CORES) % 2 == 0 else 1
    units = n // (sides * CORES) * SUM_PIECES
    part = ntok // SUM_PIECES
    bf16, f32 = jnp.bfloat16, jnp.float32
    dma = pltpu.SemaphoreType.DMA
    vmem = pl.BlockSpec(memory_space=pltpu.VMEM)
    hbm = pl.BlockSpec(memory_space=pl.ANY)
    return pl.pallas_call(
        functools.partial(kernel, n),
        out_shape=jax.ShapeDtypeStruct((ntok, block), bf16),
        in_specs=[vmem] * 5 + [hbm] * 3 + [vmem],
        out_specs=vmem,
        scratch_shapes=[
            pltpu.VMEM((width, ff), bf16),
            pltpu.VMEM((width, ff), bf16),
            pltpu.VMEM((ff, width), bf16),
            pltpu.VMEM((n, tok_dev, width + LANES), bf16),
            pltpu.VMEM((LANES, LANES), f32),
            pltpu.VMEM((ntok, ff), bf16),
            pltpu.VMEM((units, sides, part, block), f32),
            pltpu.VMEM((units, sides, part, block), bf16),
            pltpu.VMEM((units, sides, part, block), bf16),
            pltpu.VMEM((units, part, block), bf16),
            pltpu.VMEM((units, part, block), bf16),
            pltpu.VMEM((units, part, block), bf16),
            pltpu.VMEM((units, part, block), bf16),
            pltpu.VMEM((units, part, block), bf16),
            pltpu.VMEM((n, 1, ntok), f32),
            pltpu.VMEM((ntok, block), f32),
            dma((3,)),
            dma((4, n, ROW_PIECES)),
            dma((n, ROW_PIECES)),
            dma((units,)),
            dma((units,)),
            dma((units,)),
            dma((units,)),
            dma((units,)),
            dma((units,)),
            dma((units,)),
            dma((n,)),
            dma((n,)),
        ],
        compiler_params=pltpu.CompilerParams(
            collective_id=0, has_side_effects=True, vmem_limit_bytes=60 * 1024 * 1024
        ),
    )(
        tokens, routes.T, in_gain.reshape(1, width), group_router.T, expert_router.T,
        w_gate, w_up, w_down, out_gain.reshape(1, block),
    )


def solution(mesh):
    in_specs = (
        P(("grp", "ep"), None),
        P(("grp", "ep"), None),
        P(),
        P(),
        P(),
        P("ep", None, None),
        P("ep", None, None),
        P("ep", None, None),
        P("ep"),
    )
    return jax.shard_map(
        functools.partial(per_device, mesh.shape["ep"]),
        mesh=mesh, in_specs=in_specs, out_specs=P("grp", "ep"), check_vma=False,
    )
```

```python
import functools

import jax
import jax.numpy as jnp
from jax import lax
from jax.experimental import pallas as pl
from jax.experimental.pallas import tpu as pltpu
from jax.sharding import PartitionSpec as P

EPSILON = 1e-06
LANES = 128
CORES = 2
HIGH = lax.Precision.HIGHEST
UP, DOWN, SIDE, CORE = 0, 1, 2, 3
ROW_PIECES = 2
SUM_PIECES = 2
AHEAD = 3


def target_of(step, z, depth):
    mirrored = z * 2 > depth - 1
    near = jnp.where(mirrored, depth - 1 - z, z)
    lone = depth - 1 - 2 * near
    paired = step - lone
    apart = near - paired // 2
    far = jnp.where(paired % 2 == 0, near + apart, near - apart)
    found = jnp.where(step < lone, depth - 1 - step, far)
    return jnp.where(mirrored, depth - 1 - found, found)


def kernel(
    n, tokens, routes, in_gain, group_router, expert_router, w_gate, w_up, w_down, out_gain,
    out, gate_w, up_w, down_w, rows, turned, hidden, held, core_out, core_in, side_out, side_in,
    line_out, up_in, down_in, squares, total,
    load_sem, row_sent, row_got, core_sent, core_got, side_sent, side_got,
    line_sent, up_got, down_got, square_sent, square_got,
):
    tok_dev, width = tokens.shape
    experts = expert_router.shape[0]
    groups = group_router.shape[0]
    sides = 2 if (n // CORES) % 2 == 0 else 1
    plane = sides * CORES
    depth = n // plane
    ntok = n * tok_dev
    block = width // n
    ff = gate_w.shape[1]
    piece = tok_dev // ROW_PIECES
    part = ntok // SUM_PIECES
    me = lax.axis_index("ep")
    z, y, c = me // plane, (me // CORES) % sides, me % CORES
    side_step, core_step = (1 - 2 * y) * CORES, 1 - 2 * c

    loads = [
        pltpu.make_async_copy(src.at[0], dst, load_sem.at[i])
        for i, (src, dst) in enumerate(((w_gate, gate_w), (w_up, up_w), (w_down, down_w)))
    ]
    for load in loads:
        load.start()

    barrier = pltpu.get_barrier_semaphore()

    def greet(device):
        pl.semaphore_signal(
            barrier, inc=1, device_id={"ep": device}, device_id_type=pl.DeviceIdType.MESH
        )

    greet(me + core_step)
    if sides > 1:
        greet(me + side_step)

    @pl.when(z < depth - 1)
    def _():
        greet(me + plane)

    @pl.when(z > 0)
    def _():
        greet(me - plane)

    values = tokens[...].astype(jnp.float32)
    scaled = values * lax.rsqrt(jnp.mean(values * values, axis=1, keepdims=True) + EPSILON)
    normed = (scaled * in_gain[...]).astype(jnp.bfloat16)
    rows[me, :, :width] = normed
    wide = normed.astype(jnp.float32)
    across = (((1,), (1,)), ((), ()))
    group_logit = lax.dot_general(
        group_router[...], wide, across, precision=HIGH, preferred_element_type=jnp.float32
    )
    expert_logit = lax.dot_general(
        expert_router[...], wide, across, precision=HIGH, preferred_element_type=jnp.float32
    )
    group_exp = jnp.exp(group_logit)
    group_prob = group_exp / jnp.sum(group_exp, axis=0, keepdims=True)
    number = lax.broadcasted_iota(jnp.int32, (experts, tok_dev), 0)
    named = number == routes[0:1, :]
    for j in range(1, routes.shape[0]):
        named = named | (number == routes[j : j + 1, :])
    chosen = jnp.where(named, jnp.exp(expert_logit), 0.0)
    weight = chosen / jnp.sum(chosen, axis=0, keepdims=True)
    per_group = experts // groups
    of_group = jnp.zeros_like(weight)
    for g in range(groups):
        inside = (number >= g * per_group) & (number < (g + 1) * per_group)
        of_group = jnp.where(inside, group_prob[g : g + 1, :], of_group)
    weight = weight * of_group
    high = weight.astype(jnp.bfloat16).astype(jnp.float32)
    turned[...] = jnp.zeros_like(turned)
    turned[:experts, :tok_dev] = high
    turned[experts : 2 * experts, :tok_dev] = weight - high
    rows[me, :, width:] = turned[...].T[:tok_dev, :].astype(jnp.bfloat16)

    pl.semaphore_wait(barrier, sides + jnp.where(z > 0, 1, 0) + jnp.where(z < depth - 1, 1, 0))

    def row_copy(slot, p, way, device):
        at = rows.at[slot, pl.ds(p * piece, piece)]
        return pltpu.make_async_remote_copy(
            src_ref=at, dst_ref=at,
            send_sem=row_sent.at[way, slot, p], recv_sem=row_got.at[slot, p],
            device_id={"ep": device}, device_id_type=pl.DeviceIdType.MESH,
        )

    def to_side(slot, p):
        if sides > 1:
            row_copy(slot, p, SIDE, me + side_step).start()

    def to_core(slot, p):
        row_copy(slot, p, CORE, me + core_step).start()

    def to_up(slot, p):
        @pl.when(z < depth - 1)
        def _():
            row_copy(slot, p, UP, me + plane).start()

    def to_down(slot, p):
        @pl.when(z > 0)
        def _():
            row_copy(slot, p, DOWN, me - plane).start()

    def got(slot, p):
        row_copy(slot, p, CORE, me + core_step).wait_recv()

    for p in range(ROW_PIECES):
        to_up(me, p)
        to_down(me, p)
        to_side(me, p)
    for p in range(ROW_PIECES):
        to_core(me, p)

    def from_side(k, p):
        if sides > 1:
            @pl.when(z - k >= 0)
            def _():
                slot = me - k * plane + side_step
                got(slot, p)
                to_core(slot, p)

            if k > 0:
                @pl.when(z + k < depth)
                def _():
                    slot = me + k * plane + side_step
                    got(slot, p)
                    to_core(slot, p)

    for k in range(1, depth):
        for p in range(ROW_PIECES):
            @pl.when(z - k >= 0)
            def _():
                slot = me - k * plane
                got(slot, p)
                to_up(slot, p)
                to_side(slot, p)
                to_core(slot, p)

            @pl.when(z + k < depth)
            def _():
                slot = me + k * plane
                got(slot, p)
                to_down(slot, p)
                to_side(slot, p)
                to_core(slot, p)

            if k > 1:
                from_side(k - 2, p)
    for k in range(max(depth - 2, 0), depth):
        for p in range(ROW_PIECES):
            from_side(k, p)

    def from_core(k, carry):
        for p in range(ROW_PIECES):
            got(k * CORES + 1 - c, p)
        return carry

    lax.fori_loop(0, n // CORES, from_core, 0)

    loads[0].wait()
    loads[1].wait()
    lane = lax.broadcasted_iota(jnp.int32, (ntok, LANES), 1)
    mine = (lane == me) | (lane == experts + me)
    spread = rows[:, :, width:].reshape(ntok, LANES).astype(jnp.float32)
    column = jnp.sum(jnp.where(mine, spread, 0.0), axis=1, keepdims=True)
    tile = min(256, ff)

    def forward(i, carry):
        at = pl.ds(pl.multiple_of(i * tile, tile), tile)
        arrived = rows[:, :, :width].reshape(ntok, width)
        gate = jnp.dot(arrived, gate_w[:, at], preferred_element_type=jnp.float32)
        upward = jnp.dot(arrived, up_w[:, at], preferred_element_type=jnp.float32)
        silu = gate / (1.0 + jnp.exp(-gate))
        hidden[:, at] = (silu * upward * column).astype(jnp.bfloat16)
        return carry

    lax.fori_loop(0, ff // tile, forward, 0)
    loads[2].wait()

    def core_copy(j):
        return pltpu.make_async_remote_copy(
            src_ref=core_out.at[j], dst_ref=core_in.at[j],
            send_sem=core_sent.at[j], recv_sem=core_got.at[j],
            device_id={"ep": me + core_step}, device_id_type=pl.DeviceIdType.MESH,
        )

    def side_copy(j):
        return pltpu.make_async_remote_copy(
            src_ref=side_out.at[j], dst_ref=side_in.at[j],
            send_sem=side_sent.at[j], recv_sem=side_got.at[j],
            device_id={"ep": me + side_step}, device_id_type=pl.DeviceIdType.MESH,
        )

    def up_copy(target):
        return pltpu.make_async_remote_copy(
            src_ref=line_out.at[target], dst_ref=up_in.at[target],
            send_sem=line_sent.at[target], recv_sem=up_got.at[target],
            device_id={"ep": me + plane}, device_id_type=pl.DeviceIdType.MESH,
        )

    def down_copy(target):
        return pltpu.make_async_remote_copy(
            src_ref=line_out.at[target], dst_ref=down_in.at[target],
            send_sem=line_sent.at[target], recv_sem=down_got.at[target],
            device_id={"ep": me - plane}, device_id_type=pl.DeviceIdType.MESH,
        )

    units = depth * SUM_PIECES

    def produce(u):
        span = plane * block
        target = target_of(u // SUM_PIECES, z, depth)
        at = pl.ds(pl.multiple_of(target * span, span), span)
        some = pl.ds(pl.multiple_of(u % SUM_PIECES * part, part), part)
        answer = jnp.dot(hidden[some, :], down_w[:, at], preferred_element_type=jnp.float32)
        for s in range(sides):
            first = answer[:, s * CORES * block : (s * CORES + 1) * block]
            second = answer[:, (s * CORES + 1) * block : (s + 1) * CORES * block]
            held[u, s] = jnp.where(c == 0, first, second)
            core_out[u, s] = jnp.where(c == 0, second, first).astype(jnp.bfloat16)
        core_copy(u).start()

    def pair(u):
        core_copy(u).wait_recv()
        held[u, y] = held[u, y] + core_in[u, y].astype(jnp.float32)
        if sides > 1:
            far = held[u, 1 - y] + core_in[u, 1 - y].astype(jnp.float32)
            side_out[u] = far.astype(jnp.bfloat16)
            side_copy(u).start()

    ahead = min(AHEAD, units)

    def produce_only(u, carry):
        produce(u)
        return carry

    def produce_pair(u, carry):
        produce(u)
        pair(u - ahead)
        return carry

    def pair_only(u, carry):
        pair(u)
        return carry

    lax.fori_loop(0, ahead, produce_only, 0)
    lax.fori_loop(ahead, units, produce_pair, 0)
    lax.fori_loop(units - ahead, units, pair_only, 0)

    def plane_sum(u):
        found = held[u, y]
        if sides > 1:
            side_copy(u).wait_recv()
            found = found + side_in[u].astype(jnp.float32)
        return found

    def line(u, carry):
        target = target_of(u // SUM_PIECES, z, depth)
        spot = target * SUM_PIECES + u % SUM_PIECES
        held[u, y] = plane_sum(u)

        @pl.when(target > z)
        def _():
            @pl.when(z > 0)
            def _():
                up_copy(spot).wait_recv()
                held[u, y] = held[u, y] + up_in[spot].astype(jnp.float32)

            line_out[spot] = held[u, y].astype(jnp.bfloat16)
            up_copy(spot).start()

        @pl.when(target < z)
        def _():
            @pl.when(z < depth - 1)
            def _():
                down_copy(spot).wait_recv()
                held[u, y] = held[u, y] + down_in[spot].astype(jnp.float32)

            line_out[spot] = held[u, y].astype(jnp.bfloat16)
            down_copy(spot).start()

        return carry

    lax.fori_loop(0, units - SUM_PIECES, line, 0)
    for p in range(SUM_PIECES):
        spot = z * SUM_PIECES + p
        some = pl.ds(p * part, part)
        total[some, :] = plane_sum(units - SUM_PIECES + p)

        @pl.when(z > 0)
        def _():
            up_copy(spot).wait_recv()
            total[some, :] = total[some, :] + up_in[spot].astype(jnp.float32)

        @pl.when(z < depth - 1)
        def _():
            down_copy(spot).wait_recv()
            total[some, :] = total[some, :] + down_in[spot].astype(jnp.float32)

    mixed = total[...]
    summed = lax.dot_general(
        jnp.ones((8, block), jnp.float32), mixed * mixed, across,
        precision=HIGH, preferred_element_type=jnp.float32,
    )
    squares[me] = summed[0:1, :]

    def square_copy(slot, device):
        return pltpu.make_async_remote_copy(
            src_ref=squares.at[slot], dst_ref=squares.at[slot],
            send_sem=square_sent.at[device], recv_sem=square_got.at[slot],
            device_id={"ep": device}, device_id_type=pl.DeviceIdType.MESH,
        )

    def square_start(k, carry):
        square_copy(me, (me + k) % n).start()
        return carry

    lax.fori_loop(1, n, square_start, 0)

    def row_done(k, carry):
        slot = k * plane + y * CORES + c
        for p in range(ROW_PIECES):
            row_copy(slot, p, CORE, me + core_step).wait_send()
            if sides > 1:
                row_copy(slot, p, SIDE, me + side_step).wait_send()
                row_copy(slot + side_step, p, CORE, me + core_step).wait_send()

            @pl.when((k <= z) & (z < depth - 1))
            def _():
                row_copy(slot, p, UP, me + plane).wait_send()

            @pl.when((k >= z) & (z > 0))
            def _():
                row_copy(slot, p, DOWN, me - plane).wait_send()

        return carry

    lax.fori_loop(0, depth, row_done, 0)

    def sum_done(u, carry):
        k = u // SUM_PIECES
        core_copy(u).wait_send()
        if sides > 1:
            side_copy(u).wait_send()

        @pl.when(k > z)
        def _():
            up_copy(u).wait_send()

        @pl.when(k < z)
        def _():
            down_copy(u).wait_send()

        return carry

    lax.fori_loop(0, depth * SUM_PIECES, sum_done, 0)

    def square_wait(k, carry):
        square_copy((me + k) % n, (me + k) % n).wait_recv()
        return carry

    lax.fori_loop(1, n, square_wait, 0)
    power = jnp.sum(squares[...], axis=0)
    tall = jnp.broadcast_to(power, (LANES, ntok)).T[:, :block]
    scale = lax.rsqrt(tall / width + EPSILON)
    out[...] = (total[...] * scale * out_gain[...]).astype(jnp.bfloat16)

    def square_done(k, carry):
        square_copy(me, (me + k) % n).wait_send()
        return carry

    lax.fori_loop(1, n, square_done, 0)


def per_device(
    n, tokens, routes, in_gain, group_router, expert_router, w_gate, w_up, w_down, out_gain
):
    tok_dev, width = tokens.shape
    ff = w_gate.shape[2]
    ntok, block = n * tok_dev, width // n
    sides = 2 if (n // CORES) % 2 == 0 else 1
    units = n // (sides * CORES) * SUM_PIECES
    part = ntok // SUM_PIECES
    bf16, f32 = jnp.bfloat16, jnp.float32
    dma = pltpu.SemaphoreType.DMA
    vmem = pl.BlockSpec(memory_space=pltpu.VMEM)
    hbm = pl.BlockSpec(memory_space=pl.ANY)
    return pl.pallas_call(
        functools.partial(kernel, n),
        out_shape=jax.ShapeDtypeStruct((ntok, block), bf16),
        in_specs=[vmem] * 5 + [hbm] * 3 + [vmem],
        out_specs=vmem,
        scratch_shapes=[
            pltpu.VMEM((width, ff), bf16),
            pltpu.VMEM((width, ff), bf16),
            pltpu.VMEM((ff, width), bf16),
            pltpu.VMEM((n, tok_dev, width + LANES), bf16),
            pltpu.VMEM((LANES, LANES), f32),
            pltpu.VMEM((ntok, ff), bf16),
            pltpu.VMEM((units, sides, part, block), f32),
            pltpu.VMEM((units, sides, part, block), bf16),
            pltpu.VMEM((units, sides, part, block), bf16),
            pltpu.VMEM((units, part, block), bf16),
            pltpu.VMEM((units, part, block), bf16),
            pltpu.VMEM((units, part, block), bf16),
            pltpu.VMEM((units, part, block), bf16),
            pltpu.VMEM((units, part, block), bf16),
            pltpu.VMEM((n, 1, ntok), f32),
            pltpu.VMEM((ntok, block), f32),
            dma((3,)),
            dma((4, n, ROW_PIECES)),
            dma((n, ROW_PIECES)),
            dma((units,)),
            dma((units,)),
            dma((units,)),
            dma((units,)),
            dma((units,)),
            dma((units,)),
            dma((units,)),
            dma((n,)),
            dma((n,)),
        ],
        compiler_params=pltpu.CompilerParams(
            collective_id=0, has_side_effects=True, vmem_limit_bytes=60 * 1024 * 1024
        ),
    )(
        tokens, routes.T, in_gain.reshape(1, width), group_router.T, expert_router.T,
        w_gate, w_up, w_down, out_gain.reshape(1, block),
    )


def solution(mesh):
    in_specs = (
        P(("grp", "ep"), None),
        P(("grp", "ep"), None),
        P(),
        P(),
        P(),
        P("ep", None, None),
        P("ep", None, None),
        P("ep", None, None),
        P("ep"),
    )
    return jax.shard_map(
        functools.partial(per_device, mesh.shape["ep"]),
        mesh=mesh, in_specs=in_specs, out_specs=P("grp", "ep"), check_vma=False,
    )
```

```python
import functools

import jax
import jax.numpy as jnp
from jax import lax
from jax.experimental import pallas as pl
from jax.experimental.pallas import tpu as pltpu
from jax.sharding import PartitionSpec as P

EPSILON = 1e-06
LANES = 128
CORES = 2
HIGH = lax.Precision.HIGHEST
UP, DOWN, SIDE, CORE = 0, 1, 2, 3
ROW_PIECES = 2
SUM_PIECES = 2
AHEAD = 3
EARLY = 2


def target_of(step, z, depth):
    mirrored = z * 2 > depth - 1
    near = jnp.where(mirrored, depth - 1 - z, z)
    lone = depth - 1 - 2 * near
    paired = step - lone
    apart = near - paired // 2
    far = jnp.where(paired % 2 == 0, near + apart, near - apart)
    found = jnp.where(step < lone, depth - 1 - step, far)
    return jnp.where(mirrored, depth - 1 - found, found)


def kernel(
    n, tokens, routes, in_gain, group_router, expert_router, w_gate, w_up, w_down, out_gain,
    out, gate_w, up_w, down_w, rows, turned, hidden, held, core_out, core_in, side_out, side_in,
    line_out, up_in, down_in, squares, total,
    load_sem, row_sent, row_got, core_sent, core_got, side_sent, side_got,
    line_sent, up_got, down_got, square_sent, square_got,
):
    tok_dev, width = tokens.shape
    experts = expert_router.shape[0]
    groups = group_router.shape[0]
    sides = 2 if (n // CORES) % 2 == 0 else 1
    plane = sides * CORES
    depth = n // plane
    ntok = n * tok_dev
    block = width // n
    ff = gate_w.shape[1]
    piece = tok_dev // ROW_PIECES
    part = ntok // SUM_PIECES
    me = lax.axis_index("ep")
    z, y, c = me // plane, (me // CORES) % sides, me % CORES
    side_step, core_step = (1 - 2 * y) * CORES, 1 - 2 * c

    loads = [
        pltpu.make_async_copy(src.at[0], dst, load_sem.at[i])
        for i, (src, dst) in enumerate(((w_gate, gate_w), (w_up, up_w), (w_down, down_w)))
    ]
    for load in loads:
        load.start()

    barrier = pltpu.get_barrier_semaphore()

    def greet(device):
        pl.semaphore_signal(
            barrier, inc=1, device_id={"ep": device}, device_id_type=pl.DeviceIdType.MESH
        )

    greet(me + core_step)
    if sides > 1:
        greet(me + side_step)

    @pl.when(z < depth - 1)
    def _():
        greet(me + plane)

    @pl.when(z > 0)
    def _():
        greet(me - plane)

    values = tokens[...].astype(jnp.float32)
    scaled = values * lax.rsqrt(jnp.mean(values * values, axis=1, keepdims=True) + EPSILON)
    normed = (scaled * in_gain[...]).astype(jnp.bfloat16)
    rows[me, :, :width] = normed
    wide = normed.astype(jnp.float32)
    across = (((1,), (1,)), ((), ()))
    group_logit = lax.dot_general(
        group_router[...], wide, across, precision=HIGH, preferred_element_type=jnp.float32
    )
    expert_logit = lax.dot_general(
        expert_router[...], wide, across, precision=HIGH, preferred_element_type=jnp.float32
    )
    group_exp = jnp.exp(group_logit)
    group_prob = group_exp / jnp.sum(group_exp, axis=0, keepdims=True)
    number = lax.broadcasted_iota(jnp.int32, (experts, tok_dev), 0)
    named = number == routes[0:1, :]
    for j in range(1, routes.shape[0]):
        named = named | (number == routes[j : j + 1, :])
    chosen = jnp.where(named, jnp.exp(expert_logit), 0.0)
    weight = chosen / jnp.sum(chosen, axis=0, keepdims=True)
    per_group = experts // groups
    of_group = jnp.zeros_like(weight)
    for g in range(groups):
        inside = (number >= g * per_group) & (number < (g + 1) * per_group)
        of_group = jnp.where(inside, group_prob[g : g + 1, :], of_group)
    weight = weight * of_group
    high = weight.astype(jnp.bfloat16).astype(jnp.float32)
    turned[...] = jnp.zeros_like(turned)
    turned[:experts, :tok_dev] = high
    turned[experts : 2 * experts, :tok_dev] = weight - high
    rows[me, :, width:] = turned[...].T[:tok_dev, :].astype(jnp.bfloat16)

    pl.semaphore_wait(barrier, sides + jnp.where(z > 0, 1, 0) + jnp.where(z < depth - 1, 1, 0))

    def row_copy(slot, p, way, device):
        at = rows.at[slot, pl.ds(p * piece, piece)]
        return pltpu.make_async_remote_copy(
            src_ref=at, dst_ref=at,
            send_sem=row_sent.at[way, slot, p], recv_sem=row_got.at[slot, p],
            device_id={"ep": device}, device_id_type=pl.DeviceIdType.MESH,
        )

    def to_side(slot, p):
        if sides > 1:
            row_copy(slot, p, SIDE, me + side_step).start()

    def to_core(slot, p):
        row_copy(slot, p, CORE, me + core_step).start()

    def to_up(slot, p):
        @pl.when(z < depth - 1)
        def _():
            row_copy(slot, p, UP, me + plane).start()

    def to_down(slot, p):
        @pl.when(z > 0)
        def _():
            row_copy(slot, p, DOWN, me - plane).start()

    def got(slot, p):
        row_copy(slot, p, CORE, me + core_step).wait_recv()

    for p in range(ROW_PIECES):
        to_up(me, p)
        to_down(me, p)
        to_side(me, p)
    for p in range(ROW_PIECES):
        to_core(me, p)

    def from_side(k, p):
        if sides > 1:
            @pl.when(z - k >= 0)
            def _():
                slot = me - k * plane + side_step
                got(slot, p)
                to_core(slot, p)

            if k > 0:
                @pl.when(z + k < depth)
                def _():
                    slot = me + k * plane + side_step
                    got(slot, p)
                    to_core(slot, p)

    for k in range(1, depth):
        for p in range(ROW_PIECES):
            @pl.when(z - k >= 0)
            def _():
                slot = me - k * plane
                got(slot, p)
                to_up(slot, p)
                to_side(slot, p)
                to_core(slot, p)

            @pl.when(z + k < depth)
            def _():
                slot = me + k * plane
                got(slot, p)
                to_down(slot, p)
                to_side(slot, p)
                to_core(slot, p)

            if k > 1:
                from_side(k - 2, p)
    tile = min(256, ff)
    chunk = plane * tok_dev
    lane = lax.broadcasted_iota(jnp.int32, (chunk, LANES), 1)
    mine = (lane == me) | (lane == experts + me)

    def forward(i, carry):
        source = target_of(depth - 1 - i, z, depth)
        for s in range(sides):
            for p in range(ROW_PIECES):
                got(source * plane + s * CORES + 1 - c, p)
        members = pl.ds(source * plane, plane)
        some = pl.ds(pl.multiple_of(source * chunk, chunk), chunk)
        spread = rows[members, :, width:].reshape(chunk, LANES).astype(jnp.float32)
        column = jnp.sum(jnp.where(mine, spread, 0.0), axis=1, keepdims=True)
        arrived = rows[members, :, :width].reshape(chunk, width)
        for t in range(ff // tile):
            at = pl.ds(t * tile, tile)
            gate = jnp.dot(arrived, gate_w[:, at], preferred_element_type=jnp.float32)
            upward = jnp.dot(arrived, up_w[:, at], preferred_element_type=jnp.float32)
            silu = gate / (1.0 + jnp.exp(-gate))
            hidden[some, at] = (silu * upward * column).astype(jnp.bfloat16)
        return carry

    loads[0].wait()
    loads[1].wait()
    if depth > 1:
        for p in range(ROW_PIECES):
            from_side(depth - 2, p)
    early = min(EARLY, depth - 1)
    lax.fori_loop(0, early, forward, 0)
    for p in range(ROW_PIECES):
        from_side(depth - 1, p)
    lax.fori_loop(early, depth, forward, 0)
    loads[2].wait()

    def core_copy(j):
        return pltpu.make_async_remote_copy(
            src_ref=core_out.at[j], dst_ref=core_in.at[j],
            send_sem=core_sent.at[j], recv_sem=core_got.at[j],
            device_id={"ep": me + core_step}, device_id_type=pl.DeviceIdType.MESH,
        )

    def side_copy(j):
        return pltpu.make_async_remote_copy(
            src_ref=side_out.at[j], dst_ref=side_in.at[j],
            send_sem=side_sent.at[j], recv_sem=side_got.at[j],
            device_id={"ep": me + side_step}, device_id_type=pl.DeviceIdType.MESH,
        )

    def up_copy(target):
        return pltpu.make_async_remote_copy(
            src_ref=line_out.at[target], dst_ref=up_in.at[target],
            send_sem=line_sent.at[target], recv_sem=up_got.at[target],
            device_id={"ep": me + plane}, device_id_type=pl.DeviceIdType.MESH,
        )

    def down_copy(target):
        return pltpu.make_async_remote_copy(
            src_ref=line_out.at[target], dst_ref=down_in.at[target],
            send_sem=line_sent.at[target], recv_sem=down_got.at[target],
            device_id={"ep": me - plane}, device_id_type=pl.DeviceIdType.MESH,
        )

    units = depth * SUM_PIECES

    def produce(u):
        span = plane * block
        target = target_of(u // SUM_PIECES, z, depth)
        at = pl.ds(pl.multiple_of(target * span, span), span)
        some = pl.ds(pl.multiple_of(u % SUM_PIECES * part, part), part)
        answer = jnp.dot(hidden[some, :], down_w[:, at], preferred_element_type=jnp.float32)
        for s in range(sides):
            first = answer[:, s * CORES * block : (s * CORES + 1) * block]
            second = answer[:, (s * CORES + 1) * block : (s + 1) * CORES * block]
            held[u, s] = jnp.where(c == 0, first, second)
            core_out[u, s] = jnp.where(c == 0, second, first).astype(jnp.bfloat16)
        core_copy(u).start()

    def pair(u):
        core_copy(u).wait_recv()
        held[u, y] = held[u, y] + core_in[u, y].astype(jnp.float32)
        if sides > 1:
            far = held[u, 1 - y] + core_in[u, 1 - y].astype(jnp.float32)
            side_out[u] = far.astype(jnp.bfloat16)
            side_copy(u).start()

    ahead = min(AHEAD, units)

    def produce_only(u, carry):
        produce(u)
        return carry

    def produce_pair(u, carry):
        produce(u)
        pair(u - ahead)
        return carry

    def pair_only(u, carry):
        pair(u)
        return carry

    lax.fori_loop(0, ahead, produce_only, 0)
    lax.fori_loop(ahead, units, produce_pair, 0)
    lax.fori_loop(units - ahead, units, pair_only, 0)

    def plane_sum(u):
        found = held[u, y]
        if sides > 1:
            side_copy(u).wait_recv()
            found = found + side_in[u].astype(jnp.float32)
        return found

    def line(u, carry):
        target = target_of(u // SUM_PIECES, z, depth)
        spot = target * SUM_PIECES + u % SUM_PIECES
        held[u, y] = plane_sum(u)

        @pl.when(target > z)
        def _():
            @pl.when(z > 0)
            def _():
                up_copy(spot).wait_recv()
                held[u, y] = held[u, y] + up_in[spot].astype(jnp.float32)

            line_out[spot] = held[u, y].astype(jnp.bfloat16)
            up_copy(spot).start()

        @pl.when(target < z)
        def _():
            @pl.when(z < depth - 1)
            def _():
                down_copy(spot).wait_recv()
                held[u, y] = held[u, y] + down_in[spot].astype(jnp.float32)

            line_out[spot] = held[u, y].astype(jnp.bfloat16)
            down_copy(spot).start()

        return carry

    lax.fori_loop(0, units - SUM_PIECES, line, 0)
    for p in range(SUM_PIECES):
        spot = z * SUM_PIECES + p
        some = pl.ds(p * part, part)
        total[some, :] = plane_sum(units - SUM_PIECES + p)

        @pl.when(z > 0)
        def _():
            up_copy(spot).wait_recv()
            total[some, :] = total[some, :] + up_in[spot].astype(jnp.float32)

        @pl.when(z < depth - 1)
        def _():
            down_copy(spot).wait_recv()
            total[some, :] = total[some, :] + down_in[spot].astype(jnp.float32)

    mixed = total[...]
    summed = lax.dot_general(
        jnp.ones((8, block), jnp.float32), mixed * mixed, across,
        precision=HIGH, preferred_element_type=jnp.float32,
    )
    squares[me] = summed[0:1, :]

    def square_copy(slot, device):
        return pltpu.make_async_remote_copy(
            src_ref=squares.at[slot], dst_ref=squares.at[slot],
            send_sem=square_sent.at[device], recv_sem=square_got.at[slot],
            device_id={"ep": device}, device_id_type=pl.DeviceIdType.MESH,
        )

    def square_start(k, carry):
        square_copy(me, (me + k) % n).start()
        return carry

    lax.fori_loop(1, n, square_start, 0)

    def row_done(k, carry):
        slot = k * plane + y * CORES + c
        for p in range(ROW_PIECES):
            row_copy(slot, p, CORE, me + core_step).wait_send()
            if sides > 1:
                row_copy(slot, p, SIDE, me + side_step).wait_send()
                row_copy(slot + side_step, p, CORE, me + core_step).wait_send()

            @pl.when((k <= z) & (z < depth - 1))
            def _():
                row_copy(slot, p, UP, me + plane).wait_send()

            @pl.when((k >= z) & (z > 0))
            def _():
                row_copy(slot, p, DOWN, me - plane).wait_send()

        return carry

    lax.fori_loop(0, depth, row_done, 0)

    def sum_done(u, carry):
        k = u // SUM_PIECES
        core_copy(u).wait_send()
        if sides > 1:
            side_copy(u).wait_send()

        @pl.when(k > z)
        def _():
            up_copy(u).wait_send()

        @pl.when(k < z)
        def _():
            down_copy(u).wait_send()

        return carry

    lax.fori_loop(0, depth * SUM_PIECES, sum_done, 0)

    def square_wait(k, carry):
        square_copy((me + k) % n, (me + k) % n).wait_recv()
        return carry

    lax.fori_loop(1, n, square_wait, 0)
    power = jnp.sum(squares[...], axis=0)
    tall = jnp.broadcast_to(power, (LANES, ntok)).T[:, :block]
    scale = lax.rsqrt(tall / width + EPSILON)
    out[...] = (total[...] * scale * out_gain[...]).astype(jnp.bfloat16)

    def square_done(k, carry):
        square_copy(me, (me + k) % n).wait_send()
        return carry

    lax.fori_loop(1, n, square_done, 0)


def per_device(
    n, tokens, routes, in_gain, group_router, expert_router, w_gate, w_up, w_down, out_gain
):
    tok_dev, width = tokens.shape
    ff = w_gate.shape[2]
    ntok, block = n * tok_dev, width // n
    sides = 2 if (n // CORES) % 2 == 0 else 1
    units = n // (sides * CORES) * SUM_PIECES
    part = ntok // SUM_PIECES
    bf16, f32 = jnp.bfloat16, jnp.float32
    dma = pltpu.SemaphoreType.DMA
    vmem = pl.BlockSpec(memory_space=pltpu.VMEM)
    hbm = pl.BlockSpec(memory_space=pl.ANY)
    return pl.pallas_call(
        functools.partial(kernel, n),
        out_shape=jax.ShapeDtypeStruct((ntok, block), bf16),
        in_specs=[vmem] * 5 + [hbm] * 3 + [vmem],
        out_specs=vmem,
        scratch_shapes=[
            pltpu.VMEM((width, ff), bf16),
            pltpu.VMEM((width, ff), bf16),
            pltpu.VMEM((ff, width), bf16),
            pltpu.VMEM((n, tok_dev, width + LANES), bf16),
            pltpu.VMEM((LANES, LANES), f32),
            pltpu.VMEM((ntok, ff), bf16),
            pltpu.VMEM((units, sides, part, block), f32),
            pltpu.VMEM((units, sides, part, block), bf16),
            pltpu.VMEM((units, sides, part, block), bf16),
            pltpu.VMEM((units, part, block), bf16),
            pltpu.VMEM((units, part, block), bf16),
            pltpu.VMEM((units, part, block), bf16),
            pltpu.VMEM((units, part, block), bf16),
            pltpu.VMEM((units, part, block), bf16),
            pltpu.VMEM((n, 1, ntok), f32),
            pltpu.VMEM((ntok, block), f32),
            dma((3,)),
            dma((4, n, ROW_PIECES)),
            dma((n, ROW_PIECES)),
            dma((units,)),
            dma((units,)),
            dma((units,)),
            dma((units,)),
            dma((units,)),
            dma((units,)),
            dma((units,)),
            dma((n,)),
            dma((n,)),
        ],
        compiler_params=pltpu.CompilerParams(
            collective_id=0, has_side_effects=True, vmem_limit_bytes=60 * 1024 * 1024
        ),
    )(
        tokens, routes.T, in_gain.reshape(1, width), group_router.T, expert_router.T,
        w_gate, w_up, w_down, out_gain.reshape(1, block),
    )


def solution(mesh):
    in_specs = (
        P(("grp", "ep"), None),
        P(("grp", "ep"), None),
        P(),
        P(),
        P(),
        P("ep", None, None),
        P("ep", None, None),
        P("ep", None, None),
        P("ep"),
    )
    return jax.shard_map(
        functools.partial(per_device, mesh.shape["ep"]),
        mesh=mesh, in_specs=in_specs, out_specs=P("grp", "ep"), check_vma=False,
    )
```

```python
import functools

import jax
import jax.numpy as jnp
from jax import lax
from jax.experimental import pallas as pl
from jax.experimental.pallas import tpu as pltpu
from jax.sharding import PartitionSpec as P

EPSILON = 1e-06
LANES = 128
CORES = 2
HIGH = lax.Precision.HIGHEST
UP, DOWN, SIDE, CORE = 0, 1, 2, 3
ROW_PIECES = 2
SUM_PIECES = 4
AHEAD = 6
EARLY = 2


def target_of(step, z, depth):
    mirrored = z * 2 > depth - 1
    near = jnp.where(mirrored, depth - 1 - z, z)
    lone = depth - 1 - 2 * near
    paired = step - lone
    apart = near - paired // 2
    far = jnp.where(paired % 2 == 0, near + apart, near - apart)
    found = jnp.where(step < lone, depth - 1 - step, far)
    return jnp.where(mirrored, depth - 1 - found, found)


def kernel(
    n, tokens, routes, in_gain, group_router, expert_router, w_gate, w_up, w_down, out_gain,
    out, gate_w, up_w, down_w, rows, turned, hidden, held, core_out, core_in, side_out, side_in,
    line_out, up_in, down_in, squares, total,
    load_sem, row_sent, row_got, core_sent, core_got, side_sent, side_got,
    line_sent, up_got, down_got, square_sent, square_got,
):
    tok_dev, width = tokens.shape
    experts = expert_router.shape[0]
    groups = group_router.shape[0]
    sides = 2 if (n // CORES) % 2 == 0 else 1
    plane = sides * CORES
    depth = n // plane
    ntok = n * tok_dev
    block = width // n
    ff = gate_w.shape[1]
    piece = tok_dev // ROW_PIECES
    part = ntok // SUM_PIECES
    me = lax.axis_index("ep")
    z, y, c = me // plane, (me // CORES) % sides, me % CORES
    side_step, core_step = (1 - 2 * y) * CORES, 1 - 2 * c

    loads = [
        pltpu.make_async_copy(src.at[0], dst, load_sem.at[i])
        for i, (src, dst) in enumerate(((w_gate, gate_w), (w_up, up_w), (w_down, down_w)))
    ]
    for load in loads:
        load.start()

    barrier = pltpu.get_barrier_semaphore()

    def greet(device):
        pl.semaphore_signal(
            barrier, inc=1, device_id={"ep": device}, device_id_type=pl.DeviceIdType.MESH
        )

    greet(me + core_step)
    if sides > 1:
        greet(me + side_step)

    @pl.when(z < depth - 1)
    def _():
        greet(me + plane)

    @pl.when(z > 0)
    def _():
        greet(me - plane)

    values = tokens[...].astype(jnp.float32)
    scaled = values * lax.rsqrt(jnp.mean(values * values, axis=1, keepdims=True) + EPSILON)
    normed = (scaled * in_gain[...]).astype(jnp.bfloat16)
    rows[me, :, :width] = normed
    wide = normed.astype(jnp.float32)
    across = (((1,), (1,)), ((), ()))
    group_logit = lax.dot_general(
        group_router[...], wide, across, precision=HIGH, preferred_element_type=jnp.float32
    )
    expert_logit = lax.dot_general(
        expert_router[...], wide, across, precision=HIGH, preferred_element_type=jnp.float32
    )
    group_exp = jnp.exp(group_logit)
    group_prob = group_exp / jnp.sum(group_exp, axis=0, keepdims=True)
    number = lax.broadcasted_iota(jnp.int32, (experts, tok_dev), 0)
    named = number == routes[0:1, :]
    for j in range(1, routes.shape[0]):
        named = named | (number == routes[j : j + 1, :])
    chosen = jnp.where(named, jnp.exp(expert_logit), 0.0)
    weight = chosen / jnp.sum(chosen, axis=0, keepdims=True)
    per_group = experts // groups
    of_group = jnp.zeros_like(weight)
    for g in range(groups):
        inside = (number >= g * per_group) & (number < (g + 1) * per_group)
        of_group = jnp.where(inside, group_prob[g : g + 1, :], of_group)
    weight = weight * of_group
    high = weight.astype(jnp.bfloat16).astype(jnp.float32)
    turned[...] = jnp.zeros_like(turned)
    turned[:experts, :tok_dev] = high
    turned[experts : 2 * experts, :tok_dev] = weight - high
    rows[me, :, width:] = turned[...].T[:tok_dev, :].astype(jnp.bfloat16)

    pl.semaphore_wait(barrier, sides + jnp.where(z > 0, 1, 0) + jnp.where(z < depth - 1, 1, 0))

    def row_copy(slot, p, way, device):
        at = rows.at[slot, pl.ds(p * piece, piece)]
        return pltpu.make_async_remote_copy(
            src_ref=at, dst_ref=at,
            send_sem=row_sent.at[way, slot, p], recv_sem=row_got.at[slot, p],
            device_id={"ep": device}, device_id_type=pl.DeviceIdType.MESH,
        )

    def to_side(slot, p):
        if sides > 1:
            row_copy(slot, p, SIDE, me + side_step).start()

    def to_core(slot, p):
        row_copy(slot, p, CORE, me + core_step).start()

    def to_up(slot, p):
        @pl.when(z < depth - 1)
        def _():
            row_copy(slot, p, UP, me + plane).start()

    def to_down(slot, p):
        @pl.when(z > 0)
        def _():
            row_copy(slot, p, DOWN, me - plane).start()

    def got(slot, p):
        row_copy(slot, p, CORE, me + core_step).wait_recv()

    for p in range(ROW_PIECES):
        to_up(me, p)
        to_down(me, p)
        to_side(me, p)
    for p in range(ROW_PIECES):
        to_core(me, p)

    def from_side(k, p):
        if sides > 1:
            @pl.when(z - k >= 0)
            def _():
                slot = me - k * plane + side_step
                got(slot, p)
                to_core(slot, p)

            if k > 0:
                @pl.when(z + k < depth)
                def _():
                    slot = me + k * plane + side_step
                    got(slot, p)
                    to_core(slot, p)

    for k in range(1, depth):
        for p in range(ROW_PIECES):
            @pl.when(z - k >= 0)
            def _():
                slot = me - k * plane
                got(slot, p)
                to_up(slot, p)
                to_side(slot, p)
                to_core(slot, p)

            @pl.when(z + k < depth)
            def _():
                slot = me + k * plane
                got(slot, p)
                to_down(slot, p)
                to_side(slot, p)
                to_core(slot, p)

            if k > 1:
                from_side(k - 2, p)
    tile = min(256, ff)
    chunk = plane * tok_dev
    lane = lax.broadcasted_iota(jnp.int32, (chunk, LANES), 1)
    mine = (lane == me) | (lane == experts + me)

    def forward(i, carry):
        source = target_of(depth - 1 - i, z, depth)
        for s in range(sides):
            for p in range(ROW_PIECES):
                got(source * plane + s * CORES + 1 - c, p)
        members = pl.ds(source * plane, plane)
        some = pl.ds(pl.multiple_of(source * chunk, chunk), chunk)
        spread = rows[members, :, width:].reshape(chunk, LANES).astype(jnp.float32)
        column = jnp.sum(jnp.where(mine, spread, 0.0), axis=1, keepdims=True)
        arrived = rows[members, :, :width].reshape(chunk, width)
        for t in range(ff // tile):
            at = pl.ds(t * tile, tile)
            gate = jnp.dot(arrived, gate_w[:, at], preferred_element_type=jnp.float32)
            upward = jnp.dot(arrived, up_w[:, at], preferred_element_type=jnp.float32)
            silu = gate / (1.0 + jnp.exp(-gate))
            hidden[some, at] = (silu * upward * column).astype(jnp.bfloat16)
        return carry

    loads[0].wait()
    loads[1].wait()
    if depth > 1:
        for p in range(ROW_PIECES):
            from_side(depth - 2, p)
    early = min(EARLY, depth - 1)
    lax.fori_loop(0, early, forward, 0)
    for p in range(ROW_PIECES):
        from_side(depth - 1, p)
    lax.fori_loop(early, depth, forward, 0)
    loads[2].wait()

    def core_copy(j):
        return pltpu.make_async_remote_copy(
            src_ref=core_out.at[j], dst_ref=core_in.at[j],
            send_sem=core_sent.at[j], recv_sem=core_got.at[j],
            device_id={"ep": me + core_step}, device_id_type=pl.DeviceIdType.MESH,
        )

    def side_copy(j):
        return pltpu.make_async_remote_copy(
            src_ref=side_out.at[j], dst_ref=side_in.at[j],
            send_sem=side_sent.at[j], recv_sem=side_got.at[j],
            device_id={"ep": me + side_step}, device_id_type=pl.DeviceIdType.MESH,
        )

    def up_copy(target):
        return pltpu.make_async_remote_copy(
            src_ref=line_out.at[target], dst_ref=up_in.at[target],
            send_sem=line_sent.at[target], recv_sem=up_got.at[target],
            device_id={"ep": me + plane}, device_id_type=pl.DeviceIdType.MESH,
        )

    def down_copy(target):
        return pltpu.make_async_remote_copy(
            src_ref=line_out.at[target], dst_ref=down_in.at[target],
            send_sem=line_sent.at[target], recv_sem=down_got.at[target],
            device_id={"ep": me - plane}, device_id_type=pl.DeviceIdType.MESH,
        )

    units = depth * SUM_PIECES

    def produce(u):
        span = plane * block
        target = target_of(u // SUM_PIECES, z, depth)
        at = pl.ds(pl.multiple_of(target * span, span), span)
        some = pl.ds(pl.multiple_of(u % SUM_PIECES * part, part), part)
        answer = jnp.dot(hidden[some, :], down_w[:, at], preferred_element_type=jnp.float32)
        for s in range(sides):
            first = answer[:, s * CORES * block : (s * CORES + 1) * block]
            second = answer[:, (s * CORES + 1) * block : (s + 1) * CORES * block]
            held[u, s] = jnp.where(c == 0, first, second)
            core_out[u, s] = jnp.where(c == 0, second, first).astype(jnp.bfloat16)
        core_copy(u).start()

    def pair(u):
        core_copy(u).wait_recv()
        held[u, y] = held[u, y] + core_in[u, y].astype(jnp.float32)
        if sides > 1:
            far = held[u, 1 - y] + core_in[u, 1 - y].astype(jnp.float32)
            side_out[u] = far.astype(jnp.bfloat16)
            side_copy(u).start()

    ahead = min(AHEAD, units)

    def produce_only(u, carry):
        produce(u)
        return carry

    def produce_pair(u, carry):
        produce(u)
        pair(u - ahead)
        return carry

    def pair_only(u, carry):
        pair(u)
        return carry

    lax.fori_loop(0, ahead, produce_only, 0)
    lax.fori_loop(ahead, units, produce_pair, 0)
    lax.fori_loop(units - ahead, units, pair_only, 0)

    def plane_sum(u):
        found = held[u, y]
        if sides > 1:
            side_copy(u).wait_recv()
            found = found + side_in[u].astype(jnp.float32)
        return found

    def line(u, carry):
        target = target_of(u // SUM_PIECES, z, depth)
        spot = target * SUM_PIECES + u % SUM_PIECES
        held[u, y] = plane_sum(u)

        @pl.when(target > z)
        def _():
            @pl.when(z > 0)
            def _():
                up_copy(spot).wait_recv()
                held[u, y] = held[u, y] + up_in[spot].astype(jnp.float32)

            line_out[spot] = held[u, y].astype(jnp.bfloat16)
            up_copy(spot).start()

        @pl.when(target < z)
        def _():
            @pl.when(z < depth - 1)
            def _():
                down_copy(spot).wait_recv()
                held[u, y] = held[u, y] + down_in[spot].astype(jnp.float32)

            line_out[spot] = held[u, y].astype(jnp.bfloat16)
            down_copy(spot).start()

        return carry

    lax.fori_loop(0, units - SUM_PIECES, line, 0)
    for p in range(SUM_PIECES):
        spot = z * SUM_PIECES + p
        some = pl.ds(p * part, part)
        total[some, :] = plane_sum(units - SUM_PIECES + p)

        @pl.when(z > 0)
        def _():
            up_copy(spot).wait_recv()
            total[some, :] = total[some, :] + up_in[spot].astype(jnp.float32)

        @pl.when(z < depth - 1)
        def _():
            down_copy(spot).wait_recv()
            total[some, :] = total[some, :] + down_in[spot].astype(jnp.float32)

    mixed = total[...]
    summed = lax.dot_general(
        jnp.ones((8, block), jnp.float32), mixed * mixed, across,
        precision=HIGH, preferred_element_type=jnp.float32,
    )
    squares[me] = summed[0:1, :]

    def square_copy(slot, device):
        return pltpu.make_async_remote_copy(
            src_ref=squares.at[slot], dst_ref=squares.at[slot],
            send_sem=square_sent.at[device], recv_sem=square_got.at[slot],
            device_id={"ep": device}, device_id_type=pl.DeviceIdType.MESH,
        )

    def square_start(k, carry):
        square_copy(me, (me + k) % n).start()
        return carry

    lax.fori_loop(1, n, square_start, 0)

    def row_done(k, carry):
        slot = k * plane + y * CORES + c
        for p in range(ROW_PIECES):
            row_copy(slot, p, CORE, me + core_step).wait_send()
            if sides > 1:
                row_copy(slot, p, SIDE, me + side_step).wait_send()
                row_copy(slot + side_step, p, CORE, me + core_step).wait_send()

            @pl.when((k <= z) & (z < depth - 1))
            def _():
                row_copy(slot, p, UP, me + plane).wait_send()

            @pl.when((k >= z) & (z > 0))
            def _():
                row_copy(slot, p, DOWN, me - plane).wait_send()

        return carry

    lax.fori_loop(0, depth, row_done, 0)

    def sum_done(u, carry):
        k = u // SUM_PIECES
        core_copy(u).wait_send()
        if sides > 1:
            side_copy(u).wait_send()

        @pl.when(k > z)
        def _():
            up_copy(u).wait_send()

        @pl.when(k < z)
        def _():
            down_copy(u).wait_send()

        return carry

    lax.fori_loop(0, depth * SUM_PIECES, sum_done, 0)

    def square_wait(k, carry):
        square_copy((me + k) % n, (me + k) % n).wait_recv()
        return carry

    lax.fori_loop(1, n, square_wait, 0)
    power = jnp.sum(squares[...], axis=0)
    tall = jnp.broadcast_to(power, (LANES, ntok)).T[:, :block]
    scale = lax.rsqrt(tall / width + EPSILON)
    out[...] = (total[...] * scale * out_gain[...]).astype(jnp.bfloat16)

    def square_done(k, carry):
        square_copy(me, (me + k) % n).wait_send()
        return carry

    lax.fori_loop(1, n, square_done, 0)


def per_device(
    n, tokens, routes, in_gain, group_router, expert_router, w_gate, w_up, w_down, out_gain
):
    tok_dev, width = tokens.shape
    ff = w_gate.shape[2]
    ntok, block = n * tok_dev, width // n
    sides = 2 if (n // CORES) % 2 == 0 else 1
    units = n // (sides * CORES) * SUM_PIECES
    part = ntok // SUM_PIECES
    bf16, f32 = jnp.bfloat16, jnp.float32
    dma = pltpu.SemaphoreType.DMA
    vmem = pl.BlockSpec(memory_space=pltpu.VMEM)
    hbm = pl.BlockSpec(memory_space=pl.ANY)
    return pl.pallas_call(
        functools.partial(kernel, n),
        out_shape=jax.ShapeDtypeStruct((ntok, block), bf16),
        in_specs=[vmem] * 5 + [hbm] * 3 + [vmem],
        out_specs=vmem,
        scratch_shapes=[
            pltpu.VMEM((width, ff), bf16),
            pltpu.VMEM((width, ff), bf16),
            pltpu.VMEM((ff, width), bf16),
            pltpu.VMEM((n, tok_dev, width + LANES), bf16),
            pltpu.VMEM((LANES, LANES), f32),
            pltpu.VMEM((ntok, ff), bf16),
            pltpu.VMEM((units, sides, part, block), f32),
            pltpu.VMEM((units, sides, part, block), bf16),
            pltpu.VMEM((units, sides, part, block), bf16),
            pltpu.VMEM((units, part, block), bf16),
            pltpu.VMEM((units, part, block), bf16),
            pltpu.VMEM((units, part, block), bf16),
            pltpu.VMEM((units, part, block), bf16),
            pltpu.VMEM((units, part, block), bf16),
            pltpu.VMEM((n, 1, ntok), f32),
            pltpu.VMEM((ntok, block), f32),
            dma((3,)),
            dma((4, n, ROW_PIECES)),
            dma((n, ROW_PIECES)),
            dma((units,)),
            dma((units,)),
            dma((units,)),
            dma((units,)),
            dma((units,)),
            dma((units,)),
            dma((units,)),
            dma((n,)),
            dma((n,)),
        ],
        compiler_params=pltpu.CompilerParams(
            collective_id=0, has_side_effects=True, vmem_limit_bytes=60 * 1024 * 1024
        ),
    )(
        tokens, routes.T, in_gain.reshape(1, width), group_router.T, expert_router.T,
        w_gate, w_up, w_down, out_gain.reshape(1, block),
    )


def solution(mesh):
    in_specs = (
        P(("grp", "ep"), None),
        P(("grp", "ep"), None),
        P(),
        P(),
        P(),
        P("ep", None, None),
        P("ep", None, None),
        P("ep", None, None),
        P("ep"),
    )
    return jax.shard_map(
        functools.partial(per_device, mesh.shape["ep"]),
        mesh=mesh, in_specs=in_specs, out_specs=P("grp", "ep"), check_vma=False,
    )
```
